32 devices in a mesh: sp: 8 (over z, core), tp: 4 (over y, x).
Axes of the slice: x: 2, y: 2, z: 4, core: 2. Of those that a mesh axis runs over, the one named last changes fastest.
Arguments:
- routes: int32 [1536, 2], P('sp'), may hold values from 0 to 7, all different within a row; in each aligned block of 192 rows (0 to 191, 192 to 383, ...) at most 72 rows name the same one
- route_weights: float32 [1536, 2], P('sp'), may hold values from 0.2 to 1
- expert_inputs: bfloat16 [1536, 2048], P('sp', 'tp'), may hold values from -6 to 6
- out_grad: bfloat16 [1536, 2048], P('sp', 'tp'), may hold values from -6 to 6
- w_gate: bfloat16 [8, 2816, 2048], P('sp', 'tp'), may hold values from -0.125 to 0.125
- w_up: bfloat16 [8, 2816, 2048], P('sp', 'tp'), may hold values from -0.125 to 0.125
- w_down: bfloat16 [8, 2816, 2048], P('sp', 'tp'), may hold values from -0.109375 to 0.109375
- conv_u: bfloat16 [1536, 512], P('sp', 'tp'), may hold values from -6 to 6
- conv_b: bfloat16 [1536, 512], P('sp', 'tp'), may hold values from -6 to 6
- conv_c: bfloat16 [1536, 512], P('sp', 'tp'), may hold values from -6 to 6
- conv_taps: float32 [3, 512], P(None, 'tp'), may hold values from -3 to 3
- out_proj: bfloat16 [512, 2048], P('tp'), may hold values from -0.25 to 0.25
Outputs:
- grad_w_gate: bfloat16 [8, 2816, 2048], P('sp', 'tp')
- grad_w_up: bfloat16 [8, 2816, 2048], P('sp', 'tp')
- grad_w_down: bfloat16 [8, 2816, 2048], P('sp', 'tp')
- grad_input: bfloat16 [1536, 2048], P('sp', 'tp')
- grad_proj: float32 [2048, 512], P('sp', 'tp')
- grad_u: bfloat16 [1536, 512], P('sp', 'tp')
- grad_b: bfloat16 [1536, 512], P('sp', 'tp')
- grad_c: bfloat16 [1536, 512], P('sp', 'tp')
The draws below stay inside these ranges and needn't reach their ends.
Inputs may be any that keep to these rules, and one draw needn't show every extreme that they name: `routes`: each row names two different experts. In each aligned block of 192 rows no expert is named more than 72 times, a bound that some block reaches.
All inputs are finite; a program needn't handle non-finite values.
Results may differ from the reference program's by a relative error of at most 0.025.
Values may be sent and summed in bfloat16 or wider, within the bound.
A program may use at most 64 MiB of HBM per device.

```python
import math
import jax
import jax.numpy as jnp
import numpy as np
from jax import lax

D = 2048
FF = 2816
CONV_W = 512
TOK_DEV = 192
EXPERTS = 8
CAP = 72
TOKENS = 1536
N_SP = 8
N_TP = 4


def raised(result, stream_key, source, target, blocks, factor):
    def block_of(dim):
        return (jnp.arange(result.shape[dim]) // (result.shape[dim] // blocks)).reshape((-1,) + (1,) * (result.ndim - 1 - dim))

    first = jax.random.permutation(stream_key, blocks)[block_of(target)]
    far = (block_of(target) + blocks // 2) % blocks
    return jnp.where((block_of(source) == first) | (block_of(source) == far), factor * result, result)


def steps_of(stream_key, shape, split, least, high):
    factor_of = 1.0
    for dim, shards_of in split:
        steps = jax.random.uniform(jax.random.fold_in(jax.random.fold_in(stream_key, 6), dim), (shards_of,), jnp.float32, least / len(split), high / len(split))
        factor_of = factor_of * jnp.repeat(jnp.exp(steps), shape[dim] // shards_of).reshape((-1,) + (1,) * (len(shape) - 1 - dim))
    return factor_of


def assign_block(own_key, own, number, rows, count, top, limit, slope):
    sequence = jax.random.permutation(own_key, count)
    packed, usual = shares(count, rows * top, limit, slope, True), shares(count, rows * top, limit, slope, False)
    places = jnp.arange(count)

    def named(tallies, offset_by):
        used = int((tallies > 0).sum())
        fixed = max(1, used // 4)
        passed = fixed + (places - fixed + offset_by * (used - fixed)) % max(1, count - fixed)
        return jnp.zeros((count,), jnp.int32).at[sequence[jnp.where(places < fixed, places, passed)]].set(jnp.asarray(tallies, jnp.int32))

    tallies = jnp.where(number % 4 == 0, named(packed, number // 4), named(usual, number - number // 4 - 1))
    mixed = jax.random.permutation(jax.random.fold_in(own, 3), count)
    giver, receiver = mixed[0:count // 2 * 2:2], mixed[1:count // 2 * 2:2]
    margin = jnp.minimum(tallies[giver] - 1, limit - tallies[receiver]) // 2
    margin = jnp.where((giver == sequence[0]) | (receiver == sequence[0]) | (tallies[receiver] == 0), 0, jnp.maximum(margin, 0))
    passed = jax.random.randint(jax.random.fold_in(own, 4), (count // 2,), 0, 1 << 20) % (margin + 1)
    tallies = tallies.at[giver].add(-passed).at[receiver].add(passed)
    items = jnp.searchsorted(jnp.cumsum(tallies), jnp.arange(rows * top), side="right").astype(jnp.int32)
    listing = items.reshape(top, rows).T
    listing = listing[jax.random.permutation(jax.random.fold_in(own, 1), rows)]
    offset_by = jax.random.randint(jax.random.fold_in(own, 2), (rows, 1), 0, top)
    return jnp.take_along_axis(listing, (jnp.arange(top)[None, :] + offset_by) % top, axis=1)


def shares(number_of, total, limit, skew, full):
    portions = [(1 << 20) // math.isqrt(standing ** skew) + 1 for standing in range(1, number_of + 1)]
    largest = limit if full else min(limit, max(-(-total // number_of), total * portions[0] // sum(portions)))
    least = 1 if total - largest >= number_of - 1 else 0
    counts, spare = [largest] + [least] * (number_of - 1), total - largest - least * (number_of - 1)
    while spare > 0:
        movable = [i for i in range(1, number_of) if counts[i] < largest] or [i for i in range(1, number_of) if counts[i] < limit]
        whole, remaining = sum([portions[i] for i in movable]), spare
        for i in movable:
            more = min(limit - counts[i], max(1, remaining * portions[i] // whole), spare)
            counts[i] = counts[i] + more
            spare = spare - more
    return np.array(counts)


def centred(key, dims, scale, reach, pieces=(), kind=jnp.bfloat16):
    level = steps_of(key, dims, pieces, -0.22, 0.18) if pieces else 1.0
    array = jax.random.normal(key, dims, jnp.float32) * scale * level
    return jnp.minimum(jnp.maximum(array, -reach), reach).astype(kind)


def heavy_noise(stream_key, shape, scale, bound, pieces, heavy, held_as=jnp.bfloat16):
    result = scale * jax.random.normal(stream_key, shape, jnp.float32)
    if pieces:
        result = result * steps_of(stream_key, shape, pieces, -0.22, 0.18)
    return jnp.clip(raised(result, jax.random.fold_in(stream_key, 3), *heavy), -bound, bound).astype(held_as)


def setup_inputs(seed: int = 0) -> dict:
    key_of = jax.random.split(jax.random.key(seed), 13)
    routes_keys = jax.random.split(jax.random.fold_in(key_of[0], 1), TOKENS // TOK_DEV)
    routes_turns = jax.random.permutation(jax.random.fold_in(key_of[0], 3), TOKENS // TOK_DEV)
    routes = jax.vmap(lambda own, number: assign_block(jax.random.fold_in(key_of[0], 2), own, number, TOK_DEV, EXPERTS, 2, CAP, 1))(routes_keys, routes_turns).reshape((TOKENS, 2))
    route_weights = jnp.clip(0.2 + 0.8 * jax.random.uniform(key_of[1], (TOKENS, 2), jnp.float32) ** steps_of(key_of[1], (TOKENS, 2), ((0, 8),), -0.2, 0.2), 0.2, 1.0)
    expert_inputs = centred(key_of[2], (TOKENS, D), 1.0, 6.0, ((0, 8), (1, 4)))
    out_grad = heavy_noise(key_of[3], (TOKENS, D), 1.0, 6.0, ((0, 8), (1, 4)), (0, 1, 8, 2.0))
    w_gate = centred(key_of[4], (EXPERTS, FF, D), D ** -0.5, 0.125, ((0, 8), (1, 4)))
    w_up = centred(key_of[5], (EXPERTS, FF, D), D ** -0.5, 0.125, ((0, 8), (1, 4)))
    w_down = centred(key_of[6], (EXPERTS, FF, D), FF ** -0.5, 0.109375, ((0, 8), (1, 4)))
    conv_u = centred(key_of[7], (TOKENS, CONV_W), 1.0, 6.0, ((0, 8), (1, 4)))
    conv_b = centred(key_of[8], (TOKENS, CONV_W), 1.0, 6.0, ((0, 8), (1, 4)))
    conv_c = centred(key_of[9], (TOKENS, CONV_W), 1.0, 6.0, ((0, 8), (1, 4)))
    conv_taps = centred(key_of[10], (3, CONV_W), 0.6, 3.0, ((1, 4),), jnp.float32)
    out_proj = centred(key_of[11], (CONV_W, D), CONV_W ** -0.5, 0.25, ((0, 4),))
    return {"routes": routes, "route_weights": route_weights, "expert_inputs": expert_inputs, "out_grad": out_grad, "w_gate": w_gate, "w_up": w_up, "w_down": w_down, "conv_u": conv_u, "conv_b": conv_b, "conv_c": conv_c, "conv_taps": conv_taps, "out_proj": out_proj}


def contract_first(left, right):
    return lax.dot_general(left, right, (((0,), (0,)), ((), ())), preferred_element_type=jnp.float32)


def contract_last(left, right):
    return lax.dot_general(left, right, (((1,), (1,)), ((), ())), preferred_element_type=jnp.float32)


def slot_tables(routes, capacity, experts):
    flat_expert = routes.reshape(-1).astype(jnp.int32)
    columns = lax.broadcasted_iota(jnp.int32, (flat_expert.shape[0], experts), 1)
    onehot = (flat_expert[:, None] == columns).astype(jnp.int32)
    before = jnp.cumsum(onehot, axis=0) - onehot
    slot_rank = jnp.sum(before * onehot, axis=1)
    slot_index = flat_expert * capacity + slot_rank
    labels = jnp.arange(flat_expert.shape[0], dtype=jnp.int32) + 1
    slot_owner = jnp.zeros((experts * capacity,), jnp.int32).at[slot_index].set(labels)
    return slot_index, slot_owner


def expert_backward(rows, grads, gate_weight, up_weight, down_weight):
    gate_pre = contract_last(rows, gate_weight)
    up_pre = contract_last(rows, up_weight)
    gate_act = jax.nn.silu(gate_pre)
    hidden = (gate_act * up_pre).astype(jnp.bfloat16)
    grad_down = contract_first(hidden, grads).astype(jnp.bfloat16)
    grad_hidden = contract_last(grads, down_weight)
    sigma = jax.nn.sigmoid(gate_pre)
    gate_back = (grad_hidden * up_pre * sigma * (1.0 + gate_pre * (1.0 - sigma))).astype(jnp.bfloat16)
    up_back = (grad_hidden * gate_act).astype(jnp.bfloat16)
    grad_gate = contract_first(gate_back, rows).astype(jnp.bfloat16)
    grad_up = contract_first(up_back, rows).astype(jnp.bfloat16)
    return grad_gate, grad_up, grad_down, gate_back, up_back


def reference(routes, route_weights, expert_inputs, out_grad, w_gate, w_up, w_down, conv_u, conv_b, conv_c, conv_taps, out_proj):
    f32 = jnp.float32
    bf16 = jnp.bfloat16
    scaled = (route_weights[:, :, None] * out_grad.astype(f32)[:, None, :]).astype(bf16).reshape(2 * TOKENS, D)
    repeated = jnp.repeat(expert_inputs, 2, axis=0)
    slot_index, slot_owner = jax.vmap(lambda block: slot_tables(block, CAP, EXPERTS))(routes.reshape(N_SP, TOK_DEV, 2))
    offsets = jnp.arange(N_SP, dtype=jnp.int32)[:, None] * (2 * TOK_DEV)
    filled = slot_owner > 0
    sources = jnp.where(filled, slot_owner - 1 + offsets, 0).astype(jnp.int32)

    def rearrange(table):
        return table.reshape(N_SP, EXPERTS, CAP).transpose(1, 0, 2).reshape(EXPERTS, N_SP * CAP)

    sources = rearrange(sources)
    filled = rearrange(filled)
    width = FF // N_TP

    def per_expert(expert):
        picked = sources[expert]
        mask = filled[expert][:, None]
        rows = jnp.where(mask, repeated[picked], jnp.zeros((), bf16))
        grads = jnp.where(mask, scaled[picked], jnp.zeros((), bf16))
        gate_weight = w_gate[expert]
        up_weight = w_up[expert]
        grad_gate, grad_up, grad_down, gate_back, up_back = expert_backward(rows, grads, gate_weight, up_weight, w_down[expert])
        count = rows.shape[0]
        partial_value = jnp.einsum("rnf,nfd->nrd", gate_back.astype(f32).reshape(count, N_TP, width), gate_weight.astype(f32).reshape(N_TP, width, D), precision=lax.Precision.HIGHEST)
        partial_value = partial_value + jnp.einsum("rnf,nfd->nrd", up_back.astype(f32).reshape(count, N_TP, width), up_weight.astype(f32).reshape(N_TP, width, D), precision=lax.Precision.HIGHEST)
        rounded = lax.optimization_barrier(partial_value.astype(bf16))
        back_rows = jnp.sum(rounded.astype(f32), axis=0).astype(bf16)
        return grad_gate, grad_up, grad_down, back_rows

    grad_w_gate, grad_w_up, grad_w_down, back_rows = lax.map(per_expert, jnp.arange(EXPERTS, dtype=jnp.int32))
    expert_of = routes.reshape(N_SP, 2 * TOK_DEV).astype(jnp.int32)
    slot_rank = slot_index - expert_of * CAP
    position = expert_of * (N_SP * CAP) + jnp.arange(N_SP, dtype=jnp.int32)[:, None] * CAP + slot_rank
    returned = back_rows.reshape(EXPERTS * N_SP * CAP, D)[position.reshape(-1)].astype(f32).reshape(TOKENS, 2, D)
    grad_input = (out_grad.astype(f32) + returned[:, 0] + returned[:, 1]).astype(bf16)

    length = TOKENS
    mixed_in = conv_c.astype(f32) * conv_u.astype(f32)
    padded = jnp.pad(mixed_in, ((1, 1), (0, 0)))
    convolved = conv_taps[0] * padded[0:length] + conv_taps[1] * padded[1:length + 1] + conv_taps[2] * padded[2:length + 2]
    conv_out = (conv_b.astype(f32) * convolved).astype(bf16)
    grad_conv = contract_last(grad_input, out_proj)
    grad_proj = contract_first(grad_input, conv_out)
    grad_b = (grad_conv * convolved).astype(bf16)
    grad_mixed = grad_conv * conv_b.astype(f32)
    rim = jnp.pad(grad_mixed, ((1, 1), (0, 0)))
    grad_z = conv_taps[0] * rim[2:length + 2] + conv_taps[1] * rim[1:length + 1] + conv_taps[2] * rim[0:length]
    grad_c = (grad_z * conv_u.astype(f32)).astype(bf16)
    grad_u = (grad_z * conv_c.astype(f32)).astype(bf16)
    return grad_w_gate, grad_w_up, grad_w_down, grad_input, grad_proj, grad_u, grad_b, grad_c
```

```python
import functools

import jax
import jax.numpy as jnp
from jax import lax
from jax.experimental import pallas as pl
from jax.experimental.pallas import tpu as pltpu
from jax.sharding import PartitionSpec as P

MESH = pl.DeviceIdType.MESH
F32 = jnp.float32
BF16 = jnp.bfloat16


def contract_first(left, right):
    return lax.dot_general(
        left, right, (((0,), (0,)), ((), ())), preferred_element_type=jnp.float32
    )


def contract_last(left, right):
    return lax.dot_general(
        left, right, (((1,), (1,)), ((), ())), preferred_element_type=jnp.float32
    )


def loop(count, step):
    lax.fori_loop(0, count, lambda i, c: (step(i), c)[1], 0)


def enter(sizes):
    barrier = pltpu.get_barrier_semaphore()
    for axis, size in sizes:
        me = lax.axis_index(axis)

        def greet(i, axis=axis, size=size, me=me):
            pl.semaphore_signal(
                barrier,
                inc=1,
                device_id={axis: lax.rem(me + i + 1, size)},
                device_id_type=MESH,
            )

        loop(size - 1, greet)
    return lambda: pl.semaphore_wait(barrier, sum(size - 1 for _, size in sizes))


def remote(src, dst, send, recv, **where):
    return pltpu.make_async_remote_copy(
        src_ref=src,
        dst_ref=dst,
        send_sem=send,
        recv_sem=recv,
        device_id=where,
        device_id_type=MESH,
    )


def members(routes, experts):
    count = routes.shape[0]
    columns = lax.broadcasted_iota(jnp.int32, (count, experts), 1)
    first = (routes[:, 0:1] == columns).astype(F32)
    second = (routes[:, 1:2] == columns).astype(F32)
    return first, second


def triangle(count, earlier_dim):
    a = lax.broadcasted_iota(jnp.int32, (count, count), earlier_dim)
    b = lax.broadcasted_iota(jnp.int32, (count, count), 1 - earlier_dim)
    return (a < b).astype(F32).astype(BF16), (a == b).astype(F32).astype(BF16)


def dispatch_kernel(
    S, T, routes_ref, wts_ref, xin_ref, gin_ref, x_ref, g_ref,
    xs, gs, zsend, zrecv, fsend, frecv, rsend, rrecv, lsem,
):
    s, p = lax.axis_index("sp"), lax.axis_index("tp")
    cap, d = xs.shape[1], xs.shape[2]
    wait_entry = enter((("sp", S), ("tp", T)))

    routes = routes_ref[...]
    first, second = members(routes, S)
    weight = first * wts_ref[:, 0:1] + second * wts_ref[:, 1:2]
    member = (first + second).astype(BF16)
    tri, eye = triangle(routes.shape[0], 0)
    rank = contract_first(member, tri)
    named = contract_first(member, eye)
    code = jnp.where(named > 0.5, rank, -1.0).astype(jnp.int32)
    slots = lax.broadcasted_iota(jnp.int32, (cap, routes.shape[0]), 0)
    xin = xin_ref[...]
    gin = gin_ref[...].astype(F32)
    for e in range(S):
        pick = (slots == code[e : e + 1, :]).astype(F32).astype(BF16)
        xs[e] = jnp.dot(pick, xin, preferred_element_type=F32).astype(BF16)
        scaled = (weight[:, e : e + 1] * gin).astype(BF16)
        gs[e] = jnp.dot(pick, scaled, preferred_element_type=F32).astype(BF16)
    wait_entry()

    arrays = ((xs, x_ref), (gs, g_ref))

    def cols(q, half=None):
        if half is None:
            return pl.ds(pl.multiple_of(q * d, d), d)
        return pl.ds(pl.multiple_of(q * d + half * (d // 2), d // 2), d // 2)

    def origin(o):
        return lax.rem(s - o + S, S)

    def zcopy(i, o, arriving=False):
        src, out = arrays[i]
        dst = lax.rem(s + o, S)
        row = origin(o) if arriving else s
        return remote(
            src.at[dst], out.at[row, :, cols(p)], zsend.at[i, o], zrecv.at[i, o], sp=dst
        )

    locals_ = [
        pltpu.make_async_copy(src.at[s], out.at[s, :, cols(p)], lsem.at[i])
        for i, (src, out) in enumerate(arrays)
    ]
    for i in range(2):
        locals_[i].start()
        loop(S - 1, lambda k, i=i: zcopy(i, k + 1).start())

    relay = T == 4
    if relay:
        xn, yn = p + 1 - 2 * lax.rem(p, 2), lax.rem(p + 2, 4)
        partners = ((xn, xn), (yn, yn))
    else:
        partners = tuple(
            (lax.rem(p + r, T), lax.rem(p - r + T, T)) for r in range(1, T)
        )

    def fcopy(i, o, k, arriving=False):
        out = arrays[i][1]
        to, whence = partners[k]
        view = out.at[origin(o), :, cols(whence if arriving else p)]
        return remote(view, view, fsend.at[i, o, k], frecv.at[i, o, k], tp=to)

    def rcopy(i, o, k, arriving=False):
        out = arrays[i][1]
        near, far = ((xn, yn), (yn, xn))[k]
        view = out.at[origin(o), :, cols(3 - p if arriving else near, k)]
        return remote(view, view, rsend.at[i, o, k], rrecv.at[i, o, k], tp=far)

    def forward(i, o):
        @pl.when(o > 0)
        def _():
            zcopy(i, o, True).wait_recv()

        for k in range(len(partners)):
            fcopy(i, o, k).start()

    def pass_on(i, o):
        for k in range(len(partners)):
            fcopy(i, o, k, True).wait_recv()
            if relay:
                rcopy(i, o, k).start()

    for i in range(2):
        locals_[i].wait()
        forward(i, 0)
        if i == 1:
            pass_on(0, S - 1)

        def step(k, i=i):
            forward(i, k + 1)
            pass_on(i, k)

        loop(S - 1, step)
    pass_on(1, S - 1)
    for i in range(2):
        loop(S - 1, lambda k, i=i: zcopy(i, k + 1).wait_send())

        def finish(o, i=i):
            for k in range(len(partners)):
                fcopy(i, o, k).wait_send()
                if relay:
                    rcopy(i, o, k).wait_send()
                    rcopy(i, o, k, True).wait_recv()

        loop(S, finish)


def return_kernel(
    S, T, part_ref, routes_ref, grad_ref, edge_ref, own_ref, full_ref, halo_ref,
    landed, summed, back, fsend, frecv, zsend, zrecv, asend, arecv, hsend, hrecv,
):
    s, p = lax.axis_index("sp"), lax.axis_index("tp")
    cap, d = summed.shape[1], summed.shape[2]
    wait_entry = enter((("sp", S), ("tp", T)))
    wait_entry()

    def cols(q):
        return pl.ds(pl.multiple_of(q * d, d), d)

    def block(t):
        return lax.rem(s + t + 1, S)

    def fcopy(t, r):
        q = lax.rem(p + r, T)
        return remote(
            part_ref.at[block(t), :, cols(q)],
            landed.at[r - 1, block(t)],
            fsend.at[t, r - 1],
            frecv.at[t, r - 1],
            tp=q,
        )

    def zcopy(t, arriving=False):
        row = lax.rem(s - t - 1 + S, S) if arriving else s
        return remote(
            summed.at[block(t)], back.at[row], zsend.at[t], zrecv.at[t], sp=block(t)
        )

    def hcopy(k):
        to = lax.rem(s + (1 if k == 0 else S - 1), S)
        return remote(
            edge_ref.at[1 - k], halo_ref.at[k], hsend.at[k], hrecv.at[k], sp=to
        )

    def start(t):
        for r in range(1, T):
            fcopy(t, r).start()

    loop(S, start)
    for k in range(2):
        hcopy(k).start()

    def total(t):
        for r in range(1, T):
            fcopy(t, r).wait_recv()
        value = part_ref[block(t), :, cols(p)].astype(F32)
        for r in range(1, T):
            value = value + landed[r - 1, block(t)].astype(F32)
        return value.astype(BF16)

    def step(t):
        summed[block(t)] = total(t)

        @pl.when(t > 0)
        def _():
            zcopy(t - 1).start()

    loop(S - 1, step)
    back[s] = total(S - 1)
    zcopy(S - 2).start()

    routes = routes_ref[...]
    first, second = members(routes, S)
    member = (first + second).astype(BF16)
    tri, _ = triangle(routes.shape[0], 1)
    rank = jnp.dot(tri, member, preferred_element_type=F32)
    code = jnp.where(first + second > 0.5, rank, -1.0).astype(jnp.int32)
    slots = lax.broadcasted_iota(jnp.int32, (routes.shape[0], cap), 1)
    loop(S - 1, lambda t: zcopy(t, True).wait_recv())
    value = jnp.zeros((routes.shape[0], d), F32)
    for e in range(S):
        pick = (slots == code[:, e : e + 1]).astype(F32).astype(BF16)
        value = value + jnp.dot(pick, back[e], preferred_element_type=F32)
    value = (grad_ref[...].astype(F32) + value).astype(BF16)
    own_ref[...] = value
    full_ref[:, cols(p)] = value
    loop(S - 1, lambda t: zcopy(t).wait_send())

    def acopy(r, arriving=False):
        at = lax.rem(p - r + T, T) if arriving else p
        return remote(
            own_ref, full_ref.at[:, cols(at)], asend.at[r - 1], arecv.at[r - 1],
            tp=lax.rem(p + r, T),
        )

    for r in range(1, T):
        acopy(r).start()

    def finish(t):
        for r in range(1, T):
            fcopy(t, r).wait_send()

    loop(S, finish)
    for k in range(2):
        hcopy(k).wait()
    for r in range(1, T):
        acopy(r).wait_send()
        acopy(r, True).wait_recv()


def reduce_kernel(
    S, proj_ref, edge_ref, sum_ref, halo_ref, landed, psend, precv, hsend, hrecv
):
    s = lax.axis_index("sp")
    enter((("sp", S),))()

    def hcopy(k):
        to = lax.rem(s + (1 if k == 0 else S - 1), S)
        return remote(
            edge_ref.at[1 - k], halo_ref.at[k], hsend.at[k], hrecv.at[k], sp=to
        )

    def pcopy(o):
        to = lax.rem(s + o + 1, S)
        return remote(proj_ref.at[to], landed.at[o], psend.at[o], precv.at[o], sp=to)

    for k in range(2):
        hcopy(k).start()
    loop(S - 1, lambda o: pcopy(o).start())
    sum_ref[...] = proj_ref[s].astype(F32)

    def step(o):
        pcopy(o).wait_recv()
        sum_ref[...] += landed[o].astype(F32)

    loop(S - 1, step)
    loop(S - 1, lambda o: pcopy(o).wait_send())
    for k in range(2):
        hcopy(k).wait()


def vmem(count):
    return [pl.BlockSpec(memory_space=pltpu.VMEM)] * count


def params(number):
    return pltpu.CompilerParams(collective_id=number, has_side_effects=True)


def rimmed(value, halo):
    s, size = lax.axis_index("sp"), lax.axis_size("sp")
    before = jnp.where(s > 0, halo[0, -1:], 0.0)
    after = jnp.where(s < size - 1, halo[1, :1], 0.0)
    return jnp.concatenate([before, value, after], axis=0)


def edges(value):
    return jnp.stack([value[:8], value[-8:]])


def body(
    routes, route_weights, expert_inputs, out_grad, w_gate, w_up, w_down,
    conv_u, conv_b, conv_c, conv_taps, out_proj,
):
    S, T = lax.axis_size("sp"), lax.axis_size("tp")
    tokens, d = expert_inputs.shape
    channels = conv_u.shape[1]
    cap = 3 * tokens // S
    dma = pltpu.SemaphoreType.DMA
    sent = jax.ShapeDtypeStruct((S, cap, T * d), BF16)
    ways = 2 if T == 4 else T - 1
    relays = (2, S, 2) if T == 4 else (1, 1, 1)
    rows, grads = pl.pallas_call(
        functools.partial(dispatch_kernel, S, T),
        out_shape=(sent, sent),
        in_specs=vmem(4),
        out_specs=tuple(vmem(2)),
        scratch_shapes=[
            pltpu.VMEM((S, cap, d), BF16),
            pltpu.VMEM((S, cap, d), BF16),
            dma((2, S)),
            dma((2, S)),
            dma((2, S, ways)),
            dma((2, S, ways)),
            dma(relays),
            dma(relays),
            dma((2,)),
        ],
        compiler_params=params(0),
        name="dispatch",
    )(routes, route_weights, expert_inputs, out_grad)
    rows = rows.reshape(S * cap, T * d)
    grads = grads.reshape(S * cap, T * d)

    gate_weight, up_weight, down_weight = w_gate[0], w_up[0], w_down[0]
    gate_pre = contract_last(rows, gate_weight)
    up_pre = contract_last(rows, up_weight)
    sigma = jax.nn.sigmoid(gate_pre)
    gate_act = gate_pre * sigma
    hidden = (gate_act * up_pre).astype(BF16)
    grad_hidden = contract_last(grads, down_weight)
    gate_back = (
        grad_hidden * up_pre * sigma * (1.0 + gate_pre * (1.0 - sigma))
    ).astype(BF16)
    up_back = (grad_hidden * gate_act).astype(BF16)
    grad_down = contract_first(hidden, grads).astype(BF16)
    grad_gate = contract_first(gate_back, rows).astype(BF16)
    grad_up = contract_first(up_back, rows).astype(BF16)
    partial_value = jnp.dot(gate_back, gate_weight, preferred_element_type=F32) + jnp.dot(
        up_back, up_weight, preferred_element_type=F32
    )
    partial_value = partial_value.astype(BF16).reshape(S, cap, T * d)

    mixed_in = conv_c.astype(F32) * conv_u.astype(F32)
    halo_shape = jax.ShapeDtypeStruct((2, 8, channels), F32)
    grad_input, grad_full, halo = pl.pallas_call(
        functools.partial(return_kernel, S, T),
        out_shape=(
            jax.ShapeDtypeStruct((tokens, d), BF16),
            jax.ShapeDtypeStruct((tokens, T * d), BF16),
            halo_shape,
        ),
        in_specs=vmem(4),
        out_specs=tuple(vmem(3)),
        scratch_shapes=[
            pltpu.VMEM((T - 1, S, cap, d), BF16),
            pltpu.VMEM((S, cap, d), BF16),
            pltpu.VMEM((S, cap, d), BF16),
            dma((S, T - 1)),
            dma((S, T - 1)),
            dma((S,)),
            dma((S,)),
            dma((T - 1,)),
            dma((T - 1,)),
            dma((2,)),
            dma((2,)),
        ],
        compiler_params=params(1),
        name="bring_back",
    )(partial_value, routes, out_grad, edges(mixed_in))

    padded = rimmed(mixed_in, halo)
    convolved = (
        conv_taps[0] * padded[0:tokens]
        + conv_taps[1] * padded[1 : tokens + 1]
        + conv_taps[2] * padded[2 : tokens + 2]
    )
    conv_out = (conv_b.astype(F32) * convolved).astype(BF16)
    grad_conv = contract_last(grad_full, out_proj)
    grad_b = (grad_conv * convolved).astype(BF16)
    grad_mixed = grad_conv * conv_b.astype(F32)
    proj = contract_first(grad_full, conv_out).astype(BF16)
    width = proj.shape[0] // S
    proj_sum, halo = pl.pallas_call(
        functools.partial(reduce_kernel, S),
        out_shape=(jax.ShapeDtypeStruct((width, channels), F32), halo_shape),
        in_specs=vmem(2),
        out_specs=tuple(vmem(2)),
        scratch_shapes=[
            pltpu.VMEM((S - 1, width, channels), BF16),
            dma((S - 1,)),
            dma((S - 1,)),
            dma((2,)),
            dma((2,)),
        ],
        compiler_params=params(2),
        name="sum_proj",
    )(proj.reshape(S, width, channels), edges(grad_mixed))
    rim = rimmed(grad_mixed, halo)
    grad_z = (
        conv_taps[0] * rim[2 : tokens + 2]
        + conv_taps[1] * rim[1 : tokens + 1]
        + conv_taps[2] * rim[0:tokens]
    )
    grad_c = (grad_z * conv_u.astype(F32)).astype(BF16)
    grad_u = (grad_z * conv_c.astype(F32)).astype(BF16)
    return (
        grad_gate[None], grad_up[None], grad_down[None], grad_input, proj_sum,
        grad_u, grad_b, grad_c,
    )


def solution(mesh):
    in_specs = (
        P("sp", None),
        P("sp", None),
        P("sp", "tp"),
        P("sp", "tp"),
        P("sp", "tp", None),
        P("sp", "tp", None),
        P("sp", "tp", None),
        P("sp", "tp"),
        P("sp", "tp"),
        P("sp", "tp"),
        P(None, "tp"),
        P("tp", None),
    )
    out_specs = (
        P("sp", "tp", None),
        P("sp", "tp", None),
        P("sp", "tp", None),
        P("sp", "tp"),
        P("sp", "tp"),
        P("sp", "tp"),
        P("sp", "tp"),
        P("sp", "tp"),
    )
    return jax.shard_map(body, mesh=mesh, in_specs=in_specs, out_specs=out_specs, check_vma=False)
```

```python
import functools

import jax
import jax.numpy as jnp
from jax import lax
from jax.experimental import pallas as pl
from jax.experimental.pallas import tpu as pltpu
from jax.sharding import PartitionSpec as P

MESH = pl.DeviceIdType.MESH
F32 = jnp.float32
BF16 = jnp.bfloat16


def contract_first(left, right):
    return lax.dot_general(
        left, right, (((0,), (0,)), ((), ())), preferred_element_type=jnp.float32
    )


def contract_last(left, right):
    return lax.dot_general(
        left, right, (((1,), (1,)), ((), ())), preferred_element_type=jnp.float32
    )


def loop(count, step):
    lax.fori_loop(0, count, lambda i, c: (step(i), c)[1], 0)


def enter(sizes):
    barrier = pltpu.get_barrier_semaphore()
    for axis, size in sizes:
        me = lax.axis_index(axis)

        def greet(i, axis=axis, size=size, me=me):
            pl.semaphore_signal(
                barrier,
                inc=1,
                device_id={axis: lax.rem(me + i + 1, size)},
                device_id_type=MESH,
            )

        loop(size - 1, greet)
    return lambda: pl.semaphore_wait(barrier, sum(size - 1 for _, size in sizes))


def remote(src, dst, send, recv, **where):
    return pltpu.make_async_remote_copy(
        src_ref=src,
        dst_ref=dst,
        send_sem=send,
        recv_sem=recv,
        device_id=where,
        device_id_type=MESH,
    )


def slot_codes(routes, experts):
    count = routes.shape[1]
    names = lax.broadcasted_iota(jnp.int32, (experts, count), 0)
    first = (routes[0:1, :] == names).astype(F32)
    second = (routes[1:2, :] == names).astype(F32)
    early = lax.broadcasted_iota(jnp.int32, (count, count), 0)
    late = lax.broadcasted_iota(jnp.int32, (count, count), 1)
    before = (early < late).astype(F32).astype(BF16)
    rank = jnp.dot((first + second).astype(BF16), before, preferred_element_type=F32)
    code = jnp.where(first + second > 0.5, rank, -1.0).astype(jnp.int32)
    return code, first, second


def dispatch_kernel(
    S, T, routes_ref, wts_ref, xin_ref, gin_ref, x_ref, g_ref,
    xs, gs, zsend, zrecv, fsend, frecv, rsend, rrecv, lsem,
):
    s, p = lax.axis_index("sp"), lax.axis_index("tp")
    cap, d = xs.shape[1], xs.shape[2]
    wait_entry = enter((("sp", S), ("tp", T)))

    code, first, second = slot_codes(routes_ref[...], S)
    weight = first * wts_ref[0:1, :] + second * wts_ref[1:2, :]
    slots = lax.broadcasted_iota(jnp.int32, (cap, code.shape[1]), 0)
    xin = xin_ref[...]
    gin = gin_ref[...]
    for e in range(S):
        mask = slots == code[e : e + 1, :]
        pick = mask.astype(F32).astype(BF16)
        xs[e] = jnp.dot(pick, xin, preferred_element_type=F32).astype(BF16)
        held = jnp.sum(jnp.where(mask, weight[e : e + 1, :], 0.0), axis=1, keepdims=True)
        gs[e] = (held * jnp.dot(pick, gin, preferred_element_type=F32)).astype(BF16)
    wait_entry()

    arrays = ((xs, x_ref), (gs, g_ref))

    def cols(q, half=None):
        if half is None:
            return pl.ds(pl.multiple_of(q * d, d), d)
        return pl.ds(pl.multiple_of(q * d + half * (d // 2), d // 2), d // 2)

    def origin(o):
        return lax.rem(s - o + S, S)

    def zcopy(i, o, arriving=False):
        src, out = arrays[i]
        dst = lax.rem(s + o, S)
        row = origin(o) if arriving else s
        return remote(
            src.at[dst], out.at[row, :, cols(p)], zsend.at[i, o], zrecv.at[i, o], sp=dst
        )

    locals_ = [
        pltpu.make_async_copy(src.at[s], out.at[s, :, cols(p)], lsem.at[i])
        for i, (src, out) in enumerate(arrays)
    ]
    for i in range(2):
        locals_[i].start()
        loop(S - 1, lambda k, i=i: zcopy(i, k + 1).start())

    relay = T == 4
    if relay:
        xn, yn = p + 1 - 2 * lax.rem(p, 2), lax.rem(p + 2, 4)
        partners = ((xn, xn), (yn, yn))
    else:
        partners = tuple(
            (lax.rem(p + r, T), lax.rem(p - r + T, T)) for r in range(1, T)
        )

    def fcopy(i, o, k, arriving=False):
        out = arrays[i][1]
        to, whence = partners[k]
        view = out.at[origin(o), :, cols(whence if arriving else p)]
        return remote(view, view, fsend.at[i, o, k], frecv.at[i, o, k], tp=to)

    def rcopy(i, o, k, arriving=False):
        out = arrays[i][1]
        near, far = ((xn, yn), (yn, xn))[k]
        view = out.at[origin(o), :, cols(3 - p if arriving else near, k)]
        return remote(view, view, rsend.at[i, o, k], rrecv.at[i, o, k], tp=far)

    def forward(i, o):
        @pl.when(o > 0)
        def _():
            zcopy(i, o, True).wait_recv()

        for k in range(len(partners)):
            fcopy(i, o, k).start()

    def pass_on(i, o):
        for k in range(len(partners)):
            fcopy(i, o, k, True).wait_recv()
            if relay:
                rcopy(i, o, k).start()

    for i in range(2):
        locals_[i].wait()
        forward(i, 0)
        if i == 1:
            pass_on(0, S - 1)

        def step(k, i=i):
            forward(i, k + 1)
            pass_on(i, k)

        loop(S - 1, step)
    pass_on(1, S - 1)
    for i in range(2):
        loop(S - 1, lambda k, i=i: zcopy(i, k + 1).wait_send())

        def finish(o, i=i):
            for k in range(len(partners)):
                fcopy(i, o, k).wait_send()
                if relay:
                    rcopy(i, o, k).wait_send()
                    rcopy(i, o, k, True).wait_recv()

        loop(S, finish)


def return_kernel(
    S, T, part_ref, routes_ref, grad_ref, edge_ref, own_ref, full_ref, halo_ref,
    landed, met, passed, summed, back,
    fsend, frecv, bsend, brecv, zsend, zrecv, asend, arecv, hsend, hrecv,
):
    s, p = lax.axis_index("sp"), lax.axis_index("tp")
    cap, d = summed.shape[1], summed.shape[2]
    relay = T == 4
    half = d // 2
    wait_entry = enter((("sp", S), ("tp", T)))
    wait_entry()

    def cols(q):
        return pl.ds(pl.multiple_of(q * d, d), d)

    def halfcols(q, h):
        return pl.ds(pl.multiple_of(q * d + h * half, half), half)

    def block(t):
        return lax.rem(s + t + 1, S)

    def zcopy(t, arriving=False):
        row = lax.rem(s - t - 1 + S, S) if arriving else s
        return remote(
            summed.at[block(t)], back.at[row], zsend.at[t], zrecv.at[t], sp=block(t)
        )

    def hcopy(k):
        to = lax.rem(s + (1 if k == 0 else S - 1), S)
        return remote(
            edge_ref.at[1 - k], halo_ref.at[k], hsend.at[k], hrecv.at[k], sp=to
        )

    if relay:
        xn, yn = p + 1 - 2 * lax.rem(p, 2), lax.rem(p + 2, 4)
        order = ((xn, yn), (yn, xn))

        def fcopy(t, h, k):
            to = order[h][0]
            return remote(
                part_ref.at[block(t), :, halfcols(3 - p if k else to, h)],
                landed.at[h, k, block(t)],
                fsend.at[t, 2 * h + k],
                frecv.at[t, 2 * h + k],
                tp=to,
            )

        def bcopy(t, h):
            return remote(
                passed.at[h, block(t)], met.at[h, block(t)],
                bsend.at[t, h], brecv.at[t, h], tp=order[h][1],
            )

        def start(t):
            for k in (1, 0):
                for h in range(2):
                    fcopy(t, h, k).start()

        def combine(t):
            for h in range(2):
                fcopy(t, h, 1).wait_recv()
                mine = part_ref[block(t), :, halfcols(order[h][1], h)].astype(F32)
                passed[h, block(t)] = (mine + landed[h, 1, block(t)].astype(F32)).astype(
                    BF16
                )

        def total(t, out, row):
            for h in range(2):
                fcopy(t, h, 0).wait_recv()
                bcopy(t, h).wait_recv()
                mine = part_ref[block(t), :, halfcols(p, h)].astype(F32)
                mine = mine + landed[h, 0, block(t)].astype(F32)
                mine = mine + met[h, block(t)].astype(F32)
                out[row, :, h * half : (h + 1) * half] = mine.astype(BF16)

        ahead, lag = min(3, S), 2
    else:

        def fcopy(t, r):
            q = lax.rem(p + r, T)
            return remote(
                part_ref.at[block(t), :, cols(q)],
                landed.at[r - 1, block(t)],
                fsend.at[t, r - 1],
                frecv.at[t, r - 1],
                tp=q,
            )

        def start(t):
            for r in range(1, T):
                fcopy(t, r).start()

        def total(t, out, row):
            for r in range(1, T):
                fcopy(t, r).wait_recv()
            value = part_ref[block(t), :, cols(p)].astype(F32)
            for r in range(1, T):
                value = value + landed[r - 1, block(t)].astype(F32)
            out[row] = value.astype(BF16)

        ahead, lag = S, 0

    loop(ahead, start)
    for k in range(2):
        hcopy(k).start()
    code, _, _ = slot_codes(routes_ref[...], S)
    slots = lax.broadcasted_iota(jnp.int32, (cap, code.shape[1]), 0)

    def step(t):
        if relay:

            @pl.when(t < S)
            def _():
                combine(t)

        @pl.when(jnp.logical_and(t >= lag, t < S - 1 + lag))
        def _():
            total(t - lag, summed, block(t - lag))

        if relay:

            @pl.when(t < S)
            def _():
                for h in range(2):
                    bcopy(t, h).start()

            @pl.when(t + ahead < S)
            def _():
                start(t + ahead)

        @pl.when(t >= lag + 1)
        def _():
            zcopy(t - lag - 1).start()

    loop(S + lag, step)
    total(S - 1, back, s)
    loop(S - 1, lambda t: zcopy(t, True).wait_recv())
    value = jnp.zeros((code.shape[1], d), F32)
    for e in range(S):
        pick = (slots == code[e : e + 1, :]).astype(F32).astype(BF16)
        value = value + contract_first(pick, back[e])
    value = (grad_ref[...].astype(F32) + value).astype(BF16)
    own_ref[...] = value
    full_ref[:, cols(p)] = value
    loop(S - 1, lambda t: zcopy(t).wait_send())

    def acopy(r, arriving=False):
        at = lax.rem(p - r + T, T) if arriving else p
        return remote(
            own_ref, full_ref.at[:, cols(at)], asend.at[r - 1], arecv.at[r - 1],
            tp=lax.rem(p + r, T),
        )

    for r in range(1, T):
        acopy(r).start()

    def finish(t):
        if relay:
            for h in range(2):
                fcopy(t, h, 0).wait_send()
                fcopy(t, h, 1).wait_send()
                bcopy(t, h).wait_send()
        else:
            for r in range(1, T):
                fcopy(t, r).wait_send()

    loop(S, finish)
    for k in range(2):
        hcopy(k).wait()
    for r in range(1, T):
        acopy(r).wait_send()
        acopy(r, True).wait_recv()


def reduce_kernel(
    S, proj_ref, edge_ref, sum_ref, halo_ref,
    given, pairs, landed, gsend, grecv, psend, precv, hsend, hrecv,
):
    s = lax.axis_index("sp")
    n = S // 2
    z, c = s // 2, lax.rem(s, 2)
    enter((("sp", S),))()

    def hcopy(k):
        to = lax.rem(s + (1 if k == 0 else S - 1), S)
        return remote(
            edge_ref.at[1 - k], halo_ref.at[k], hsend.at[k], hrecv.at[k], sp=to
        )

    def at(o):
        return lax.rem(z + o, n)

    def gcopy(o):
        return remote(
            proj_ref.at[2 * at(o) + 1 - c], given.at[at(o)],
            gsend.at[o], grecv.at[o], sp=s + 1 - 2 * c,
        )

    def pcopy(o):
        return remote(
            pairs.at[at(o)], landed.at[o - 1], psend.at[o - 1], precv.at[o - 1],
            sp=2 * at(o) + c,
        )

    for k in range(2):
        hcopy(k).start()
    for o in range(1, n + 1):
        gcopy(o % n).start()

    def pair(o):
        gcopy(o).wait_recv()
        return proj_ref[2 * at(o) + c].astype(F32) + given[at(o)].astype(F32)

    for o in range(1, n):
        pairs[at(o)] = pair(o).astype(BF16)
        if o > 1:
            pcopy(o - 1).start()
    sum_ref[...] = pair(0)
    pcopy(n - 1).start()
    for o in range(1, n):
        pcopy(o).wait_recv()
        sum_ref[...] += landed[o - 1].astype(F32)
    for o in range(n):
        gcopy(o).wait_send()
        if o > 0:
            pcopy(o).wait_send()
    for k in range(2):
        hcopy(k).wait()


def vmem(count):
    return [pl.BlockSpec(memory_space=pltpu.VMEM)] * count


def params(number):
    return pltpu.CompilerParams(collective_id=number, has_side_effects=True)


def rimmed(value, halo):
    s, size = lax.axis_index("sp"), lax.axis_size("sp")
    before = jnp.where(s > 0, halo[0, -1:], 0.0)
    after = jnp.where(s < size - 1, halo[1, :1], 0.0)
    return jnp.concatenate([before, value, after], axis=0)


def edges(value):
    return jnp.stack([value[:8], value[-8:]])


def body(
    routes, route_weights, expert_inputs, out_grad, w_gate, w_up, w_down,
    conv_u, conv_b, conv_c, conv_taps, out_proj,
):
    S, T = lax.axis_size("sp"), lax.axis_size("tp")
    tokens, d = expert_inputs.shape
    channels = conv_u.shape[1]
    cap = 3 * tokens // S
    dma = pltpu.SemaphoreType.DMA
    sent = jax.ShapeDtypeStruct((S, cap, T * d), BF16)
    ways = 2 if T == 4 else T - 1
    relays = (2, S, 2) if T == 4 else (1, 1, 1)
    rows, grads = pl.pallas_call(
        functools.partial(dispatch_kernel, S, T),
        out_shape=(sent, sent),
        in_specs=vmem(4),
        out_specs=tuple(vmem(2)),
        scratch_shapes=[
            pltpu.VMEM((S, cap, d), BF16),
            pltpu.VMEM((S, cap, d), BF16),
            dma((2, S)),
            dma((2, S)),
            dma((2, S, ways)),
            dma((2, S, ways)),
            dma(relays),
            dma(relays),
            dma((2,)),
        ],
        compiler_params=params(0),
        name="dispatch",
    )(routes.T, route_weights.T, expert_inputs, out_grad)
    rows = rows.reshape(S * cap, T * d)
    grads = grads.reshape(S * cap, T * d)

    gate_weight, up_weight, down_weight = w_gate[0], w_up[0], w_down[0]
    gate_pre = contract_last(rows, gate_weight)
    up_pre = contract_last(rows, up_weight)
    sigma = jax.nn.sigmoid(gate_pre)
    gate_act = gate_pre * sigma
    hidden = (gate_act * up_pre).astype(BF16)
    grad_hidden = contract_last(grads, down_weight)
    gate_back = (
        grad_hidden * up_pre * sigma * (1.0 + gate_pre * (1.0 - sigma))
    ).astype(BF16)
    up_back = (grad_hidden * gate_act).astype(BF16)
    grad_down = contract_first(hidden, grads).astype(BF16)
    grad_gate = contract_first(gate_back, rows).astype(BF16)
    grad_up = contract_first(up_back, rows).astype(BF16)
    partial_value = jnp.dot(gate_back, gate_weight, preferred_element_type=F32) + jnp.dot(
        up_back, up_weight, preferred_element_type=F32
    )
    partial_value = partial_value.astype(BF16).reshape(S, cap, T * d)

    if T == 4:
        pieces = 4
        shapes = ((2, 2, S, cap, d // 2), (2, S, cap, d // 2), (2, S, cap, d // 2))
    else:
        pieces = T - 1
        shapes = ((T - 1, S, cap, d), (8, 128), (8, 128))
    landing = [pltpu.VMEM(shape, BF16) for shape in shapes]
    mixed_in = conv_c.astype(F32) * conv_u.astype(F32)
    halo_shape = jax.ShapeDtypeStruct((2, 8, channels), F32)
    grad_input, grad_full, halo = pl.pallas_call(
        functools.partial(return_kernel, S, T),
        out_shape=(
            jax.ShapeDtypeStruct((tokens, d), BF16),
            jax.ShapeDtypeStruct((tokens, T * d), BF16),
            halo_shape,
        ),
        in_specs=vmem(4),
        out_specs=tuple(vmem(3)),
        scratch_shapes=[
            *landing,
            pltpu.VMEM((S, cap, d), BF16),
            pltpu.VMEM((S, cap, d), BF16),
            dma((S, pieces)),
            dma((S, pieces)),
            dma(relays[1:]),
            dma(relays[1:]),
            dma((S,)),
            dma((S,)),
            dma((T - 1,)),
            dma((T - 1,)),
            dma((2,)),
            dma((2,)),
        ],
        compiler_params=params(1),
        name="bring_back",
    )(partial_value, routes.T, out_grad, edges(mixed_in))

    padded = rimmed(mixed_in, halo)
    convolved = (
        conv_taps[0] * padded[0:tokens]
        + conv_taps[1] * padded[1 : tokens + 1]
        + conv_taps[2] * padded[2 : tokens + 2]
    )
    conv_out = (conv_b.astype(F32) * convolved).astype(BF16)
    grad_conv = contract_last(grad_full, out_proj)
    grad_b = (grad_conv * convolved).astype(BF16)
    grad_mixed = grad_conv * conv_b.astype(F32)
    proj = contract_first(grad_full, conv_out).astype(BF16)
    width = proj.shape[0] // S
    proj_sum, halo = pl.pallas_call(
        functools.partial(reduce_kernel, S),
        out_shape=(jax.ShapeDtypeStruct((width, channels), F32), halo_shape),
        in_specs=vmem(2),
        out_specs=tuple(vmem(2)),
        scratch_shapes=[
            pltpu.VMEM((S // 2, width, channels), BF16),
            pltpu.VMEM((S // 2, width, channels), BF16),
            pltpu.VMEM((S // 2 - 1, width, channels), BF16),
            dma((S // 2,)),
            dma((S // 2,)),
            dma((S // 2 - 1,)),
            dma((S // 2 - 1,)),
            dma((2,)),
            dma((2,)),
        ],
        compiler_params=params(2),
        name="sum_proj",
    )(proj.reshape(S, width, channels), edges(grad_mixed))
    rim = rimmed(grad_mixed, halo)
    grad_z = (
        conv_taps[0] * rim[2 : tokens + 2]
        + conv_taps[1] * rim[1 : tokens + 1]
        + conv_taps[2] * rim[0:tokens]
    )
    grad_c = (grad_z * conv_u.astype(F32)).astype(BF16)
    grad_u = (grad_z * conv_c.astype(F32)).astype(BF16)
    return (
        grad_gate[None], grad_up[None], grad_down[None], grad_input, proj_sum,
        grad_u, grad_b, grad_c,
    )


def solution(mesh):
    in_specs = (
        P("sp", None),
        P("sp", None),
        P("sp", "tp"),
        P("sp", "tp"),
        P("sp", "tp", None),
        P("sp", "tp", None),
        P("sp", "tp", None),
        P("sp", "tp"),
        P("sp", "tp"),
        P("sp", "tp"),
        P(None, "tp"),
        P("tp", None),
    )
    out_specs = (
        P("sp", "tp", None),
        P("sp", "tp", None),
        P("sp", "tp", None),
        P("sp", "tp"),
        P("sp", "tp"),
        P("sp", "tp"),
        P("sp", "tp"),
        P("sp", "tp"),
    )
    return jax.shard_map(body, mesh=mesh, in_specs=in_specs, out_specs=out_specs, check_vma=False)
```
